32 devices in a mesh: ep: 8 (over z, core), tp: 4 (over y, x).
Axes of the slice: x: 2, y: 2, z: 4, core: 2. Of those that a mesh axis runs over, the one named last changes fastest.
Arguments:
- mixer_input: bfloat16 [1024, 2048], P('ep'), may hold values from -6 to 6
- mixer_gain: float32 [2048], replicated, may hold values from 0.1 to 1.9
- glu_value_weight: bfloat16 [512, 2048], P('tp'), may hold values from -0.125 to 0.125
- glu_gate_weight: bfloat16 [512, 2048], P('tp'), may hold values from -0.125 to 0.125
- conv_taps: float32 [512, 31], P('tp'), may hold values from -1 to 1
- conv_bias: float32 [512], P('tp'), may hold values from -3 to 3
- channel_gain: float32 [512], replicated, may hold values from 0.1 to 1.9
- channel_shift: float32 [512], replicated, may hold values from -3 to 3
- mixer_out_weight: bfloat16 [512, 2048], P(None, 'tp'), may hold values from -0.25 to 0.25
- expert_input: bfloat16 [2048, 2048], P('ep'), may hold values from -6 to 6
- expert_gain: float32 [2048], replicated, may hold values from 0.1 to 1.9
- routes: int32 [2048, 2], P('ep'), may hold values from 0 to 7, all different within a row; in each aligned block of 256 rows (0 to 255, 256 to 511, ...) at most 96 rows name the same one
- route_logits: float32 [2048, 2], P('ep'), may hold values from -8 to 8
- gate_weight: bfloat16 [8, 2048, 4096], P('ep', None, 'tp'), may hold values from -0.125 to 0.125
- up_weight: bfloat16 [8, 2048, 4096], P('ep', None, 'tp'), may hold values from -0.125 to 0.125
- down_weight: bfloat16 [8, 4096, 2048], P('ep', 'tp'), may hold values from -0.09375 to 0.09375
Outputs:
- mixer_output: bfloat16 [1024, 2048], P('ep', 'tp')
- expert_output: bfloat16 [2048, 2048], P('ep', 'tp')
The draws below stay inside these ranges and needn't reach their ends.
Inputs may be any that keep to these rules, and one draw needn't show every extreme that they name: `routes`: the 2 entries of a row differ. Among the rows of one index of ep, no expert is named by more than 96 rows, a bound that some block reaches.
All inputs are finite; a program needn't handle non-finite values.
Results may differ from the reference program's by a relative error of at most 0.015.
Values may be sent and summed in bfloat16 or wider, within the bound.
A program may use at most 64 MiB of HBM per device.

```python
import math
import jax
import jax.numpy as jnp
import numpy as np
from jax import lax

D = 2048
CH = 512
FF = 4096
KERNEL = 31
TOP = 2
ROWS_B = 256
EXPERTS = 8
CAP = 96
TOKENS_A = 1024
TOKENS_B = 2048
N_EP = 8
N_TP = 4


def shard_levels(own_key, extent, pieces, least, high):
    def one(axis_at, blocks):
        steps = jax.random.uniform(jax.random.fold_in(jax.random.fold_in(own_key, 6), axis_at), (blocks,), jnp.float32, least / len(pieces), high / len(pieces))
        return jnp.repeat(jnp.exp(steps), extent[axis_at] // blocks).reshape((-1,) + (1,) * (len(extent) - axis_at - 1))

    factor_of = one(*pieces[0])
    for cut in pieces[1:]:
        factor_of = factor_of * one(*cut)
    return factor_of


def assign_block(rng, own, number, rows, count, top, limit, skew):
    order = jax.random.permutation(rng, count)
    crowded, usual = portions_of(count, rows * top, limit, skew, True), portions_of(count, rows * top, limit, skew, False)
    places = jnp.arange(count)

    def named(sizes, rotation):
        used = int((sizes > 0).sum())
        fixed = max(1, used // 4)
        moved = fixed + (places - fixed + rotation * (used - fixed)) % max(1, count - fixed)
        return jnp.zeros((count,), jnp.int32).at[order[jnp.where(places < fixed, places, moved)]].set(jnp.asarray(sizes, jnp.int32))

    sizes = jnp.where(number % 4 == 0, named(crowded, number // 4), named(usual, number - number // 4 - 1))
    mixed = jax.random.permutation(jax.random.fold_in(own, 3), count)
    giver, sink = mixed[0:count // 2 * 2:2], mixed[1:count // 2 * 2:2]
    room = jnp.minimum(sizes[giver] - 1, limit - sizes[sink]) // 2
    room = jnp.where((giver == order[0]) | (sink == order[0]) | (sizes[sink] == 0), 0, jnp.maximum(room, 0))
    moved = jax.random.randint(jax.random.fold_in(own, 4), (count // 2,), 0, 1 << 20) % (room + 1)
    sizes = sizes.at[giver].add(-moved).at[sink].add(moved)
    labels = jnp.searchsorted(jnp.cumsum(sizes), jnp.arange(rows * top), side="right").astype(jnp.int32)
    listing = labels.reshape(top, rows).T
    listing = listing[jax.random.permutation(jax.random.fold_in(own, 1), rows)]
    rotation = jax.random.randint(jax.random.fold_in(own, 2), (rows, 1), 0, top)
    return jnp.take_along_axis(listing, (jnp.arange(top)[None, :] + rotation) % top, axis=1)


def portions_of(number_of, total, most, lean, full):
    portions = [(1 << 20) // math.isqrt(grade ** lean) + 1 for grade in range(1, number_of + 1)]
    largest = most if full else min(most, max(-(-total // number_of), total * portions[0] // sum(portions)))
    least = 1 if total - largest >= number_of - 1 else 0
    counts, surplus = [largest] + [least] * (number_of - 1), total - largest - least * (number_of - 1)
    while surplus > 0:
        free = [i for i in range(1, number_of) if counts[i] < largest] or [i for i in range(1, number_of) if counts[i] < most]
        pool, budget = sum([portions[i] for i in free]), surplus
        for i in free:
            extra = min(most - counts[i], max(1, budget * portions[i] // pool), surplus)
            counts[i] = counts[i] + extra
            surplus = surplus - extra
    return np.array(counts)


def noise(rng, dims, width, reach, split=(), kind=jnp.bfloat16):
    array = jax.random.normal(rng, dims, jnp.float32) * width
    if len(split) > 0:
        array = shard_levels(rng, dims, split, -0.22, 0.18) * array
    return jnp.clip(array, min=-reach, max=reach).astype(kind)


def setup_inputs(seed: int = 0) -> dict:
    key_list = jax.random.split(jax.random.key(seed), 17)
    mixer_input = noise(key_list[0], (TOKENS_A, D), 1.0, 6.0, ((0, 8),))
    mixer_gain = jnp.clip(1.0 + 0.18 * jax.random.normal(key_list[1], (D,), jnp.float32), 0.1, 1.9)
    glu_value_weight = noise(key_list[2], (CH, D), D ** -0.5, 0.125, ((0, 4),))
    glu_gate_weight = noise(key_list[3], (CH, D), D ** -0.5, 0.125, ((0, 4),))
    conv_taps = noise(key_list[4], (CH, KERNEL), KERNEL ** -0.5, 1.0, ((0, 4),), jnp.float32)
    conv_bias = noise(key_list[5], (CH,), 0.5, 3.0, ((0, 4),), jnp.float32)
    channel_gain = jnp.clip(1.0 + 0.18 * jax.random.normal(key_list[6], (CH,), jnp.float32), 0.1, 1.9)
    channel_shift = noise(key_list[7], (CH,), 0.5, 3.0, (), jnp.float32)
    mixer_out_weight = noise(key_list[8], (CH, D), CH ** -0.5, 0.25, ((1, 4),))
    expert_input = noise(key_list[9], (TOKENS_B, D), 1.0, 6.0, ((0, 8),))
    expert_gain = jnp.clip(1.0 + 0.18 * jax.random.normal(key_list[10], (D,), jnp.float32), 0.1, 1.9)
    routes_keys = jax.random.split(jax.random.fold_in(key_list[11], 1), TOKENS_B // ROWS_B)
    routes_turns = jax.random.permutation(jax.random.fold_in(key_list[11], 3), TOKENS_B // ROWS_B)
    routes = jax.vmap(lambda own, number: assign_block(jax.random.fold_in(key_list[11], 2), own, number, ROWS_B, EXPERTS, TOP, CAP, 1))(routes_keys, routes_turns).reshape((TOKENS_B, TOP))
    route_logits = noise(key_list[12], (TOKENS_B, TOP), 1.5, 8.0, ((0, 8),), jnp.float32)
    gate_weight = noise(key_list[13], (EXPERTS, D, FF), D ** -0.5, 0.125, ((0, 8), (2, 4)))
    up_weight = noise(key_list[14], (EXPERTS, D, FF), D ** -0.5, 0.125, ((0, 8), (2, 4)))
    down_weight = noise(key_list[15], (EXPERTS, FF, D), FF ** -0.5, 0.09375, ((0, 8), (1, 4)))
    return {"mixer_input": mixer_input, "mixer_gain": mixer_gain, "glu_value_weight": glu_value_weight, "glu_gate_weight": glu_gate_weight, "conv_taps": conv_taps, "conv_bias": conv_bias, "channel_gain": channel_gain, "channel_shift": channel_shift, "mixer_out_weight": mixer_out_weight, "expert_input": expert_input, "expert_gain": expert_gain, "routes": routes, "route_logits": route_logits, "gate_weight": gate_weight, "up_weight": up_weight, "down_weight": down_weight}


norm_eps = 1e-06

def rms_rows(row_block, gain_vec):
    row_values = row_block.astype(jnp.float32)
    inv_scale = lax.rsqrt(lax.optimization_barrier(jnp.mean(row_values * row_values, axis=-1, keepdims=True)) + norm_eps)
    return (row_values * inv_scale * gain_vec[None, :]).astype(jnp.bfloat16)

def mixer_half(mixer_input, mixer_gain, glu_value_weight, glu_gate_weight, conv_taps, conv_bias, channel_gain, channel_shift, mixer_out_weight):
    normed = rms_rows(mixer_input, mixer_gain)
    contract = (((1,), (1,)), ((), ()))
    glu_value = lax.dot_general(normed, glu_value_weight, contract, preferred_element_type=jnp.float32)
    glu_gate = lax.dot_general(normed, glu_gate_weight, contract, preferred_element_type=jnp.float32)
    gated_rows = (glu_value * jax.nn.sigmoid(glu_gate)).astype(jnp.bfloat16)
    padded = jnp.pad(gated_rows.astype(jnp.float32), ((KERNEL - 1, 0), (0, 0)))
    conv_sum = jnp.zeros((TOKENS_A, CH), jnp.float32)
    for offset in range(KERNEL):
        conv_sum = conv_sum + padded[offset:offset + TOKENS_A] * conv_taps[:, offset][None, :]
    conv_out = (conv_sum + conv_bias[None, :]).astype(jnp.bfloat16)
    chan_values = conv_out.astype(jnp.float32)
    chan_mean = lax.optimization_barrier(jnp.mean(chan_values, axis=1, keepdims=True))
    centered = chan_values - chan_mean
    variance = lax.optimization_barrier(jnp.mean(centered * centered, axis=1, keepdims=True))
    shaped = centered * lax.rsqrt(variance + norm_eps) * channel_gain[None, :] + channel_shift[None, :]
    activated = jax.nn.silu(shaped).astype(jnp.bfloat16)
    return jnp.dot(activated, mixer_out_weight, preferred_element_type=jnp.float32).astype(jnp.bfloat16)

def expert_half(expert_input, expert_gain, routes, route_logits, gate_weight, up_weight, down_weight):
    normed = rms_rows(expert_input, expert_gain)
    assigned = routes.reshape(N_EP, ROWS_B * TOP)
    matches = (assigned[:, :, None] == jnp.arange(EXPERTS, dtype=jnp.int32)[None, None, :]).astype(jnp.int32)
    earlier = jnp.cumsum(matches, axis=1) - matches
    slot_index = lax.optimization_barrier(jnp.sum(earlier * matches, axis=2))
    source_dev = jnp.arange(N_EP, dtype=jnp.int32)[:, None]
    slot_place = (source_dev * CAP + slot_index).reshape(-1).astype(jnp.int32)
    owner_row = (source_dev * ROWS_B + jnp.arange(ROWS_B * TOP, dtype=jnp.int32)[None, :] // TOP).reshape(-1).astype(jnp.int32)
    expert_ids = assigned.reshape(-1)
    slot_owner = jnp.full((EXPERTS, N_EP * CAP), TOKENS_B, jnp.int32).at[expert_ids, slot_place].set(owner_row)

    def one_expert(packed):
        slot_rows, gate_mat, up_mat, down_mat = packed
        rows_in = jnp.take(normed, slot_rows, axis=0, mode='fill', fill_value=0)
        gate_acts = jnp.dot(rows_in, gate_mat, preferred_element_type=jnp.float32)
        up_acts = jnp.dot(rows_in, up_mat, preferred_element_type=jnp.float32)
        hidden = (jax.nn.silu(gate_acts) * up_acts).astype(jnp.bfloat16)
        hid_groups = hidden.reshape(N_EP * CAP, N_TP, FF // N_TP).astype(jnp.float32)
        down_groups = down_mat.reshape(N_TP, FF // N_TP, D).astype(jnp.float32)
        partial_value = jnp.einsum('sgf,gfd->gsd', hid_groups, down_groups).astype(jnp.bfloat16)
        return lax.optimization_barrier(jnp.sum(partial_value.astype(jnp.float32), axis=0)).astype(jnp.bfloat16)
    results = lax.map(one_expert, (slot_owner, gate_weight, up_weight, down_weight))
    picked = results[expert_ids, slot_place].astype(jnp.float32).reshape(TOKENS_B, TOP, D)
    first_weight = jax.nn.sigmoid(route_logits[:, 0] - route_logits[:, 1])
    second_weight = jax.nn.sigmoid(route_logits[:, 1] - route_logits[:, 0])
    combined = picked[:, 0] * first_weight[:, None] + picked[:, 1] * second_weight[:, None]
    return combined.astype(jnp.bfloat16)

def reference(mixer_input, mixer_gain, glu_value_weight, glu_gate_weight, conv_taps, conv_bias, channel_gain, channel_shift, mixer_out_weight, expert_input, expert_gain, routes, route_logits, gate_weight, up_weight, down_weight):
    mixer_output = mixer_half(mixer_input, mixer_gain, glu_value_weight, glu_gate_weight, conv_taps, conv_bias, channel_gain, channel_shift, mixer_out_weight)
    expert_output = expert_half(expert_input, expert_gain, routes, route_logits, gate_weight, up_weight, down_weight)
    return (mixer_output, expert_output)
```

```python
import functools

import jax
import jax.numpy as jnp
from jax import lax
from jax.experimental import pallas as pl
from jax.experimental.pallas import tpu as pltpu
from jax.sharding import PartitionSpec as P

norm_eps = 1e-06
MESH = pl.DeviceIdType.MESH
f32 = jnp.float32
bf16 = jnp.bfloat16


def shifted(value, axis, steps):
    count = lax.axis_size(axis)
    first, last = (max(0, -steps), min(count, count - steps))
    return lax.ppermute(value, axis, [(source, source + steps) for source in range(first, last)])


def rms_rows(row_block, gain_vec):
    row_values = row_block.astype(jnp.float32)
    inv_scale = lax.rsqrt(jnp.mean(row_values * row_values, axis=-1, keepdims=True) + norm_eps)
    return (row_values * inv_scale * gain_vec[None, :]).astype(jnp.bfloat16)


def expert_kernel(
    n_ep, n_tp, cap,
    x_ref, gain_ref, routes_ref, routes_t_ref, logits_ref, gate_hbm, up_hbm, down_hbm,
    out_ref,
    gate_w, up_w, down_w, normed, out_part, out_pair, xin, hidden, part, own_part, got, summed, ret,
    w_sem, z_send, z_recv, ag_send, ag_recv, rs_send, rs_recv, y_send, y_recv,
):
    e = lax.axis_index("ep")
    t = lax.axis_index("tp")
    n_z = n_ep // 2
    z = e // 2
    c = e % 2
    mate = e + 1 - 2 * c
    width = out_part.shape[1]
    rows, feat = x_ref.shape
    pair = 2 * cap
    slots = n_ep * cap
    peers = n_tp - 1

    weight_copies = [
        pltpu.make_async_copy(gate_hbm.at[0], gate_w, w_sem.at[0]),
        pltpu.make_async_copy(up_hbm.at[0], up_w, w_sem.at[1]),
        pltpu.make_async_copy(down_hbm.at[0], down_w, w_sem.at[2]),
    ]
    for copy in weight_copies:
        copy.start()

    barrier = pltpu.get_barrier_semaphore()
    for o in range(1, n_ep):
        pl.semaphore_signal(barrier, inc=1, device_id=((e + o) % n_ep, t), device_id_type=MESH)
    for o in range(1, n_tp):
        pl.semaphore_signal(barrier, inc=1, device_id=(e, (t + o) % n_tp), device_id_type=MESH)

    def rows_of(index, count):
        return pl.ds(pl.multiple_of(index * count, count), count)

    def cols_of(index, count):
        return pl.ds(pl.multiple_of(index * count, count), count)

    values = x_ref[...].astype(f32)
    scale = lax.rsqrt(jnp.mean(values * values, axis=-1, keepdims=True) + norm_eps)
    normed[...] = (values * scale * gain_ref[...]).astype(bf16)

    lanes = lax.broadcasted_iota(jnp.int32, (rows, 128), 1)
    m0 = (lanes == routes_ref[:, 0:1]).astype(f32)
    m1 = (lanes == routes_ref[:, 1:2]).astype(f32)
    ri = lax.broadcasted_iota(jnp.int32, (rows, rows), 0)
    ci = lax.broadcasted_iota(jnp.int32, (rows, rows), 1)
    lower = (ci < ri).astype(f32).astype(bf16)
    upper = (ri < ci).astype(f32).astype(bf16)
    count = jnp.dot(lower, (m0 + m1).astype(bf16), preferred_element_type=f32)
    base = count + (lanes * cap).astype(f32)
    place0 = jnp.sum(base * m0, axis=1, keepdims=True).astype(jnp.int32)
    place1 = jnp.sum(base * m1, axis=1, keepdims=True).astype(jnp.int32)
    subs = lax.broadcasted_iota(jnp.int32, (128, rows), 0)
    t0 = (subs == routes_t_ref[0:1, :]).astype(f32)
    t1 = (subs == routes_t_ref[1:2, :]).astype(f32)
    count_t = jnp.dot((t0 + t1).astype(bf16), upper, preferred_element_type=f32)
    base_t = count_t + (subs * cap).astype(f32)
    row0 = jnp.sum(base_t * t0, axis=0, keepdims=True).astype(jnp.int32)
    row1 = jnp.sum(base_t * t1, axis=0, keepdims=True).astype(jnp.int32)

    def pick(first, size):
        at = lax.broadcasted_iota(jnp.int32, (size, rows), 0) + first
        return ((at == row0) | (at == row1)).astype(f32).astype(bf16)

    out_part[...] = jnp.dot(
        pick(0, slots), normed[:, cols_of(t, width)], preferred_element_type=f32
    ).astype(bf16)

    pl.semaphore_wait(barrier, n_ep - 1 + peers)

    z_copies = []
    for k in range(1, n_z):
        for cc in range(2):
            dest = ((z + k) % n_z) * 2 + cc
            copy = pltpu.make_async_remote_copy(
                src_ref=out_part.at[rows_of(dest, cap), :],
                dst_ref=xin.at[rows_of(e, cap), cols_of(t, width)],
                send_sem=z_send.at[2 * k + cc],
                recv_sem=z_recv.at[2 * k + c],
                device_id=(dest, t),
                device_id_type=MESH,
            )
            copy.start()
            z_copies.append(copy)

    out_pair[...] = jnp.dot(
        pick(mate * cap, cap), normed[...], preferred_element_type=f32
    ).astype(bf16)
    mate_copy = pltpu.make_async_remote_copy(
        src_ref=out_pair,
        dst_ref=xin.at[rows_of(e, cap), :],
        send_sem=z_send.at[0],
        recv_sem=z_recv.at[0],
        device_id=(mate, t),
        device_id_type=MESH,
    )
    mate_copy.start()
    xin[rows_of(e, cap), :] = jnp.dot(
        pick(e * cap, cap), normed[...], preferred_element_type=f32
    ).astype(bf16)

    def source_chip(k):
        return (z + n_z - k) % n_z

    ag_copies = []

    def gather(k):
        chip = source_chip(k)
        for cc in range(2):
            block = xin.at[rows_of(chip * 2 + cc, cap), cols_of(t, width)]
            pltpu.make_async_remote_copy(
                src_ref=block, dst_ref=block, send_sem=z_send.at[2 * k + cc],
                recv_sem=z_recv.at[2 * k + cc], device_id=(mate, t), device_id_type=MESH,
            ).wait_recv()
        block = xin.at[rows_of(chip, pair), cols_of(t, width)]
        for o in range(1, n_tp):
            copy = pltpu.make_async_remote_copy(
                src_ref=block, dst_ref=block, send_sem=ag_send.at[k * peers + o - 1],
                recv_sem=ag_recv.at[k * peers + o - 1],
                device_id=(e, (t + o) % n_tp), device_id_type=MESH,
            )
            copy.start()
            ag_copies.append(copy)

    def gathered(k):
        chip = source_chip(k)
        for o in range(1, n_tp):
            block = xin.at[rows_of(chip, pair), cols_of((t + n_tp - o) % n_tp, width)]
            pltpu.make_async_remote_copy(
                src_ref=block, dst_ref=block, send_sem=ag_send.at[k * peers + o - 1],
                recv_sem=ag_recv.at[k * peers + o - 1],
                device_id=(mate, t), device_id_type=MESH,
            ).wait_recv()

    units = gate_w.shape[1]
    tile = min(units, 256)
    rs_copies = []
    y_copies = []

    def up_half(k):
        here = rows_of(source_chip(k), pair)

        def one(j, carry):
            cols = cols_of(j, tile)
            rows_in = xin[here, :]
            g = jnp.dot(rows_in, gate_w[:, cols], preferred_element_type=f32)
            u = jnp.dot(rows_in, up_w[:, cols], preferred_element_type=f32)
            hidden[:, cols] = (g * jax.nn.sigmoid(g) * u).astype(bf16)
            return carry

        lax.fori_loop(0, units // tile, one, 0)

    def down_half(k):
        for o in range(1, n_tp):
            peer = (t + o) % n_tp
            at = k * peers + o - 1
            part[at] = jnp.dot(
                hidden[...], down_w[:, cols_of(peer, width)], preferred_element_type=f32
            ).astype(bf16)
            copy = pltpu.make_async_remote_copy(
                src_ref=part.at[at], dst_ref=got.at[at], send_sem=rs_send.at[at],
                recv_sem=rs_recv.at[at], device_id=(e, peer), device_id_type=MESH,
            )
            copy.start()
            rs_copies.append(copy)
        own_part[k] = jnp.dot(
            hidden[...], down_w[:, cols_of(t, width)], preferred_element_type=f32
        ).astype(bf16)

    def finish(k):
        chip = source_chip(k)
        total = own_part[k].astype(f32)
        for o in range(1, n_tp):
            at = k * peers + o - 1
            pltpu.make_async_remote_copy(
                src_ref=part.at[at], dst_ref=got.at[at], send_sem=rs_send.at[at],
                recv_sem=rs_recv.at[at], device_id=(mate, t), device_id_type=MESH,
            ).wait_recv()
            total = total + got[at].astype(f32)
        summed[k] = total.astype(bf16)
        if k == 0:
            copy = pltpu.make_async_remote_copy(
                src_ref=summed.at[0, rows_of(1 - c, cap), :], dst_ref=ret.at[rows_of(e, cap), :],
                send_sem=y_send.at[0], recv_sem=y_recv.at[0],
                device_id=(mate, t), device_id_type=MESH,
            )
            copy.start()
            y_copies.append(copy)
            ret[rows_of(e, cap), :] = summed[0, rows_of(c, cap), :]
            return
        for cc in range(2):
            copy = pltpu.make_async_remote_copy(
                src_ref=summed.at[k, pl.ds(cc * cap, cap), :], dst_ref=ret.at[rows_of(e, cap), :],
                send_sem=y_send.at[2 * k + cc], recv_sem=y_recv.at[2 * k + c],
                device_id=(chip * 2 + cc, t), device_id_type=MESH,
            )
            copy.start()
            y_copies.append(copy)

    if n_z > 1:
        gather(1)
    mate_block = xin.at[rows_of(mate, cap), :]
    pltpu.make_async_remote_copy(
        src_ref=mate_block, dst_ref=mate_block, send_sem=z_send.at[0], recv_sem=z_recv.at[0],
        device_id=(mate, t), device_id_type=MESH,
    ).wait_recv()
    weight_copies[0].wait()
    weight_copies[1].wait()
    for k in range(n_z):
        if k > 0:
            gathered(k)
        up_half(k)
        if k == 0:
            weight_copies[2].wait()
        if k + 2 < n_z:
            gather(k + 2)
        down_half(k)
        if k > 0:
            finish(k - 1)
    finish(n_z - 1)

    block = ret.at[rows_of(mate, cap), :]
    pltpu.make_async_remote_copy(
        src_ref=block, dst_ref=block, send_sem=y_send.at[0], recv_sem=y_recv.at[0],
        device_id=(mate, t), device_id_type=MESH,
    ).wait_recv()
    for k in range(1, n_z):
        for cc in range(2):
            block = ret.at[rows_of(((z + k) % n_z) * 2 + cc, cap), :]
            pltpu.make_async_remote_copy(
                src_ref=block, dst_ref=block, send_sem=y_send.at[2 * k + cc],
                recv_sem=y_recv.at[2 * k + cc], device_id=(mate, t), device_id_type=MESH,
            ).wait_recv()
    at = lax.broadcasted_iota(jnp.int32, (rows, slots), 1)
    l0 = logits_ref[:, 0:1]
    l1 = logits_ref[:, 1:2]
    first = jnp.dot(
        (at == place0).astype(f32).astype(bf16), ret[...], preferred_element_type=f32
    )
    second = jnp.dot(
        (at == place1).astype(f32).astype(bf16), ret[...], preferred_element_type=f32
    )
    out_ref[...] = (
        first * jax.nn.sigmoid(l0 - l1) + second * jax.nn.sigmoid(l1 - l0)
    ).astype(bf16)
    for copy in [mate_copy] + z_copies + ag_copies + rs_copies + y_copies:
        copy.wait_send()


def experts(expert_input, expert_gain, routes, route_logits, gate_weight, up_weight, down_weight):
    n_ep, n_tp = lax.axis_size("ep"), lax.axis_size("tp")
    rows, feat = expert_input.shape
    cap = 3 * rows // n_ep
    cap = -(-cap // 16) * 16
    units = gate_weight.shape[2]
    width = feat // n_tp
    n_z, peers, pair, slots = n_ep // 2, n_tp - 1, 2 * cap, n_ep * cap
    vmem = pl.BlockSpec(memory_space=pltpu.VMEM)
    hbm = pl.BlockSpec(memory_space=pl.ANY)
    dma = pltpu.SemaphoreType.DMA
    return pl.pallas_call(
        functools.partial(expert_kernel, n_ep, n_tp, cap),
        out_shape=jax.ShapeDtypeStruct((rows, width), bf16),
        in_specs=[vmem] * 5 + [hbm] * 3,
        out_specs=vmem,
        scratch_shapes=[
            pltpu.VMEM((feat, units), bf16),
            pltpu.VMEM((feat, units), bf16),
            pltpu.VMEM((units, feat), bf16),
            pltpu.VMEM((rows, feat), bf16),
            pltpu.VMEM((slots, width), bf16),
            pltpu.VMEM((cap, feat), bf16),
            pltpu.VMEM((slots, feat), bf16),
            pltpu.VMEM((pair, units), bf16),
            pltpu.VMEM((n_z * peers, pair, width), bf16),
            pltpu.VMEM((n_z, pair, width), bf16),
            pltpu.VMEM((n_z * peers, pair, width), bf16),
            pltpu.VMEM((n_z, pair, width), bf16),
            pltpu.VMEM((slots, width), bf16),
            dma((3,)),
            dma((n_ep,)),
            dma((n_ep,)),
            dma((n_z * peers,)),
            dma((n_z * peers,)),
            dma((n_z * peers,)),
            dma((n_z * peers,)),
            dma((n_ep,)),
            dma((n_ep,)),
        ],
        compiler_params=pltpu.CompilerParams(
            collective_id=0, has_side_effects=True, vmem_limit_bytes=48 * 1024 * 1024
        ),
        cost_estimate=pl.CostEstimate(
            flops=6 * slots * feat * units, bytes_accessed=6 * feat * units, transcendentals=0
        ),
    )(
        expert_input, expert_gain[None, :], routes, routes.T, route_logits,
        gate_weight, up_weight, down_weight,
    )


def on_device(
    mixer_input,
    mixer_gain,
    glu_value_weight,
    glu_gate_weight,
    conv_taps,
    conv_bias,
    channel_gain,
    channel_shift,
    mixer_out_weight,
    expert_input,
    expert_gain,
    routes,
    route_logits,
    gate_weight,
    up_weight,
    down_weight,
):
    normed_a = rms_rows(mixer_input, mixer_gain)
    contract = (((1,), (1,)), ((), ()))
    glu_value = lax.dot_general(
        glu_value_weight, normed_a, contract, preferred_element_type=jnp.float32
    )
    glu_gate = lax.dot_general(
        glu_gate_weight, normed_a, contract, preferred_element_type=jnp.float32
    )
    gated_rows = (glu_value * jax.nn.sigmoid(glu_gate)).astype(jnp.bfloat16)
    row_count = gated_rows.shape[1]
    reach_back = conv_taps.shape[1] - 1
    tail_rows = shifted(gated_rows[:, row_count - reach_back :], "ep", 1)
    padded = jnp.concatenate([tail_rows, gated_rows], axis=1).astype(jnp.float32)
    conv_sum = jnp.zeros(gated_rows.shape, jnp.float32)
    for offset in range(reach_back + 1):
        conv_sum = (
            conv_sum + conv_taps[:, offset : offset + 1] * padded[:, offset : offset + row_count]
        )
    conv_out = (conv_sum + conv_bias[:, None]).astype(jnp.bfloat16)
    all_channels = lax.all_gather(conv_out, "tp", axis=0, tiled=True)
    chan_values = all_channels.astype(jnp.float32)
    chan_mean = jnp.mean(chan_values, axis=0, keepdims=True)
    centered = chan_values - chan_mean
    variance = jnp.mean(centered * centered, axis=0, keepdims=True)
    shaped = (
        centered * lax.rsqrt(variance + norm_eps) * channel_gain[:, None] + channel_shift[:, None]
    )
    activated = jax.nn.silu(shaped).astype(jnp.bfloat16)
    mixer_output = lax.dot_general(
        activated, mixer_out_weight, (((0,), (0,)), ((), ())), preferred_element_type=jnp.float32
    ).astype(jnp.bfloat16)
    expert_output = experts(
        expert_input, expert_gain, routes, route_logits, gate_weight, up_weight, down_weight
    )
    return (mixer_output, expert_output)


def solution(mesh):
    in_specs = (
        P("ep", None),
        P(),
        P("tp", None),
        P("tp", None),
        P("tp", None),
        P("tp"),
        P(),
        P(),
        P(None, "tp"),
        P("ep", None),
        P(),
        P("ep", None),
        P("ep", None),
        P("ep", None, "tp"),
        P("ep", None, "tp"),
        P("ep", "tp", None),
    )
    out_specs = (P("ep", "tp"), P("ep", "tp"))
    return jax.shard_map(
        on_device, mesh=mesh, in_specs=in_specs, out_specs=out_specs, check_vma=False
    )
```

```python
import functools

import jax
import jax.numpy as jnp
from jax import lax
from jax.experimental import pallas as pl
from jax.experimental.pallas import tpu as pltpu
from jax.sharding import PartitionSpec as P

norm_eps = 1e-06
MESH = pl.DeviceIdType.MESH
f32 = jnp.float32
bf16 = jnp.bfloat16


def step_kernel(
    n_ep, n_tp, cap,
    x_ref, gain_ref, routes_ref, routes_t_ref, logits_ref, gate_hbm, up_hbm, down_hbm,
    mix_gain_ref, taps_ref, bias_ref, chan_gain_ref, chan_shift_ref,
    mix_hbm, value_hbm, glu_gate_hbm, mix_out_hbm,
    out_ref, mix_out_ref,
    gate_w, up_w, down_w, normed, out_part, out_pair, xin, hidden, part, own_part, got, summed, ret,
    w_sem, z_send, z_recv, ag_send, ag_recv, rs_send, rs_recv, y_send, y_recv,
    mix_in, value_w, glu_gate_w, mix_out_w, gated, tail, padded, conv_own, channels,
    tail_sem, c_send, c_recv,
):
    e = lax.axis_index("ep")
    t = lax.axis_index("tp")
    n_z = n_ep // 2
    z = e // 2
    c = e % 2
    mate = e + 1 - 2 * c
    width = out_part.shape[1]
    rows, feat = x_ref.shape
    pair = 2 * cap
    slots = n_ep * cap
    peers = n_tp - 1

    weight_copies = [
        pltpu.make_async_copy(gate_hbm.at[0], gate_w, w_sem.at[0]),
        pltpu.make_async_copy(up_hbm.at[0], up_w, w_sem.at[1]),
        pltpu.make_async_copy(down_hbm.at[0], down_w, w_sem.at[2]),
    ]
    mix_copies = [
        pltpu.make_async_copy(mix_hbm, mix_in, w_sem.at[3]),
        pltpu.make_async_copy(value_hbm, value_w, w_sem.at[4]),
        pltpu.make_async_copy(glu_gate_hbm, glu_gate_w, w_sem.at[5]),
        pltpu.make_async_copy(mix_out_hbm, mix_out_w, w_sem.at[6]),
    ]
    for copy in mix_copies[:3] + weight_copies + mix_copies[3:]:
        copy.start()

    barrier = pltpu.get_barrier_semaphore()
    for o in range(1, n_ep):
        pl.semaphore_signal(barrier, inc=1, device_id=((e + o) % n_ep, t), device_id_type=MESH)
    for o in range(1, n_tp):
        pl.semaphore_signal(barrier, inc=1, device_id=(e, (t + o) % n_tp), device_id_type=MESH)

    def rows_of(index, count):
        return pl.ds(pl.multiple_of(index * count, count), count)

    def cols_of(index, count):
        return pl.ds(pl.multiple_of(index * count, count), count)

    values = x_ref[...].astype(f32)
    scale = lax.rsqrt(jnp.mean(values * values, axis=-1, keepdims=True) + norm_eps)
    normed[...] = (values * scale * gain_ref[...]).astype(bf16)

    lanes = lax.broadcasted_iota(jnp.int32, (rows, 128), 1)
    m0 = (lanes == routes_ref[:, 0:1]).astype(f32)
    m1 = (lanes == routes_ref[:, 1:2]).astype(f32)
    ri = lax.broadcasted_iota(jnp.int32, (rows, rows), 0)
    ci = lax.broadcasted_iota(jnp.int32, (rows, rows), 1)
    lower = (ci < ri).astype(f32).astype(bf16)
    upper = (ri < ci).astype(f32).astype(bf16)
    count = jnp.dot(lower, (m0 + m1).astype(bf16), preferred_element_type=f32)
    base = count + (lanes * cap).astype(f32)
    place0 = jnp.sum(base * m0, axis=1, keepdims=True).astype(jnp.int32)
    place1 = jnp.sum(base * m1, axis=1, keepdims=True).astype(jnp.int32)
    subs = lax.broadcasted_iota(jnp.int32, (128, rows), 0)
    t0 = (subs == routes_t_ref[0:1, :]).astype(f32)
    t1 = (subs == routes_t_ref[1:2, :]).astype(f32)
    count_t = jnp.dot((t0 + t1).astype(bf16), upper, preferred_element_type=f32)
    base_t = count_t + (subs * cap).astype(f32)
    row0 = jnp.sum(base_t * t0, axis=0, keepdims=True).astype(jnp.int32)
    row1 = jnp.sum(base_t * t1, axis=0, keepdims=True).astype(jnp.int32)

    def pick(first, size):
        at = lax.broadcasted_iota(jnp.int32, (size, rows), 0) + first
        return ((at == row0) | (at == row1)).astype(f32).astype(bf16)

    out_part[...] = jnp.dot(
        pick(0, slots), normed[:, cols_of(t, width)], preferred_element_type=f32
    ).astype(bf16)

    pl.semaphore_wait(barrier, n_ep - 1 + peers)

    z_copies = []
    for k in range(1, n_z):
        for cc in range(2):
            dest = ((z + k) % n_z) * 2 + cc
            copy = pltpu.make_async_remote_copy(
                src_ref=out_part.at[rows_of(dest, cap), :],
                dst_ref=xin.at[rows_of(e, cap), cols_of(t, width)],
                send_sem=z_send.at[2 * k + cc],
                recv_sem=z_recv.at[2 * k + c],
                device_id=(dest, t),
                device_id_type=MESH,
            )
            copy.start()
            z_copies.append(copy)

    out_pair[...] = jnp.dot(
        pick(mate * cap, cap), normed[...], preferred_element_type=f32
    ).astype(bf16)
    mate_copy = pltpu.make_async_remote_copy(
        src_ref=out_pair,
        dst_ref=xin.at[rows_of(e, cap), :],
        send_sem=z_send.at[0],
        recv_sem=z_recv.at[0],
        device_id=(mate, t),
        device_id_type=MESH,
    )
    mate_copy.start()
    xin[rows_of(e, cap), :] = jnp.dot(
        pick(e * cap, cap), normed[...], preferred_element_type=f32
    ).astype(bf16)

    def source_chip(k):
        return (z + n_z - k) % n_z

    ag_copies = []

    def gather(k):
        chip = source_chip(k)
        for cc in range(2):
            block = xin.at[rows_of(chip * 2 + cc, cap), cols_of(t, width)]
            pltpu.make_async_remote_copy(
                src_ref=block, dst_ref=block, send_sem=z_send.at[2 * k + cc],
                recv_sem=z_recv.at[2 * k + cc], device_id=(mate, t), device_id_type=MESH,
            ).wait_recv()
        block = xin.at[rows_of(chip, pair), cols_of(t, width)]
        for o in range(1, n_tp):
            copy = pltpu.make_async_remote_copy(
                src_ref=block, dst_ref=block, send_sem=ag_send.at[k * peers + o - 1],
                recv_sem=ag_recv.at[k * peers + o - 1],
                device_id=(e, (t + o) % n_tp), device_id_type=MESH,
            )
            copy.start()
            ag_copies.append(copy)

    def gathered(k):
        chip = source_chip(k)
        for o in range(1, n_tp):
            block = xin.at[rows_of(chip, pair), cols_of((t + n_tp - o) % n_tp, width)]
            pltpu.make_async_remote_copy(
                src_ref=block, dst_ref=block, send_sem=ag_send.at[k * peers + o - 1],
                recv_sem=ag_recv.at[k * peers + o - 1],
                device_id=(mate, t), device_id_type=MESH,
            ).wait_recv()

    units = gate_w.shape[1]
    tile = min(units, 256)
    rs_copies = []
    y_copies = []

    def up_half(k):
        here = rows_of(source_chip(k), pair)

        def one(j, carry):
            cols = cols_of(j, tile)
            rows_in = xin[here, :]
            g = jnp.dot(rows_in, gate_w[:, cols], preferred_element_type=f32)
            u = jnp.dot(rows_in, up_w[:, cols], preferred_element_type=f32)
            hidden[:, cols] = (g * jax.nn.sigmoid(g) * u).astype(bf16)
            return carry

        lax.fori_loop(0, units // tile, one, 0)

    def down_half(k):
        for o in range(1, n_tp):
            peer = (t + o) % n_tp
            at = k * peers + o - 1
            part[at] = jnp.dot(
                hidden[...], down_w[:, cols_of(peer, width)], preferred_element_type=f32
            ).astype(bf16)
            copy = pltpu.make_async_remote_copy(
                src_ref=part.at[at], dst_ref=got.at[at], send_sem=rs_send.at[at],
                recv_sem=rs_recv.at[at], device_id=(e, peer), device_id_type=MESH,
            )
            copy.start()
            rs_copies.append(copy)
        own_part[k] = jnp.dot(
            hidden[...], down_w[:, cols_of(t, width)], preferred_element_type=f32
        ).astype(bf16)

    def finish(k):
        chip = source_chip(k)
        total = own_part[k].astype(f32)
        for o in range(1, n_tp):
            at = k * peers + o - 1
            pltpu.make_async_remote_copy(
                src_ref=part.at[at], dst_ref=got.at[at], send_sem=rs_send.at[at],
                recv_sem=rs_recv.at[at], device_id=(mate, t), device_id_type=MESH,
            ).wait_recv()
            total = total + got[at].astype(f32)
        summed[k] = total.astype(bf16)
        if k == 0:
            copy = pltpu.make_async_remote_copy(
                src_ref=summed.at[0, rows_of(1 - c, cap), :], dst_ref=ret.at[rows_of(e, cap), :],
                send_sem=y_send.at[0], recv_sem=y_recv.at[0],
                device_id=(mate, t), device_id_type=MESH,
            )
            copy.start()
            y_copies.append(copy)
            ret[rows_of(e, cap), :] = summed[0, rows_of(c, cap), :]
            return
        for cc in range(2):
            copy = pltpu.make_async_remote_copy(
                src_ref=summed.at[k, pl.ds(cc * cap, cap), :], dst_ref=ret.at[rows_of(e, cap), :],
                send_sem=y_send.at[2 * k + cc], recv_sem=y_recv.at[2 * k + c],
                device_id=(chip * 2 + cc, t), device_id_type=MESH,
            )
            copy.start()
            y_copies.append(copy)

    taken, chans = gated.shape
    keep = tail.shape[0]
    reach = taps_ref.shape[0] - 1
    conv_copies = []

    def tail_copy():
        return pltpu.make_async_remote_copy(
            src_ref=gated.at[pl.ds(taken - keep, keep), :], dst_ref=tail,
            send_sem=tail_sem.at[0], recv_sem=tail_sem.at[1],
            device_id=((e + 1) % n_ep, t), device_id_type=MESH,
        )

    def glu():
        for copy in mix_copies[:3]:
            copy.wait()
        mixed = mix_in[...].astype(f32)
        inv = lax.rsqrt(jnp.mean(mixed * mixed, axis=-1, keepdims=True) + norm_eps)
        normed_a = (mixed * inv * mix_gain_ref[...]).astype(bf16)
        contract = (((1,), (1,)), ((), ()))
        value = lax.dot_general(normed_a, value_w[...], contract, preferred_element_type=f32)
        gate = lax.dot_general(normed_a, glu_gate_w[...], contract, preferred_element_type=f32)
        gated[...] = (value * jax.nn.sigmoid(gate)).astype(bf16)
        copy = tail_copy()
        copy.start()
        conv_copies.append(copy)

    def convolve():
        tail_copy().wait_recv()
        before = tail[...].astype(f32)
        padded[pl.ds(0, keep), :] = jnp.where(e > 0, before, jnp.zeros_like(before))
        padded[pl.ds(keep, taken), :] = gated[...].astype(f32)
        total = jnp.zeros((taken, chans), f32)
        for offset in range(reach + 1):
            shift = keep - reach + offset
            total = total + padded[pl.ds(shift, taken), :] * taps_ref[offset : offset + 1, :]
        done = (total + bias_ref[...]).astype(bf16)
        conv_own[...] = done
        channels[t] = done
        for o in range(1, n_tp):
            copy = pltpu.make_async_remote_copy(
                src_ref=conv_own, dst_ref=channels.at[t],
                send_sem=c_send.at[o - 1], recv_sem=c_recv.at[o - 1],
                device_id=(e, (t + o) % n_tp), device_id_type=MESH,
            )
            copy.start()
            conv_copies.append(copy)

    def mixer_end():
        for o in range(1, n_tp):
            pltpu.make_async_remote_copy(
                src_ref=conv_own, dst_ref=channels.at[(t + n_tp - o) % n_tp],
                send_sem=c_send.at[o - 1], recv_sem=c_recv.at[o - 1],
                device_id=(mate, t), device_id_type=MESH,
            ).wait_recv()
        mix_copies[3].wait()
        chan_values = jnp.concatenate([channels[i].astype(f32) for i in range(n_tp)], axis=1)
        centered = chan_values - jnp.mean(chan_values, axis=1, keepdims=True)
        variance = jnp.mean(centered * centered, axis=1, keepdims=True)
        shaped = (
            centered * lax.rsqrt(variance + norm_eps) * chan_gain_ref[...] + chan_shift_ref[...]
        )
        activated = (shaped * jax.nn.sigmoid(shaped)).astype(bf16)
        mix_out_ref[...] = jnp.dot(
            activated, mix_out_w[...], preferred_element_type=f32
        ).astype(bf16)

    glu()
    if n_z > 1:
        gather(1)
    mate_block = xin.at[rows_of(mate, cap), :]
    pltpu.make_async_remote_copy(
        src_ref=mate_block, dst_ref=mate_block, send_sem=z_send.at[0], recv_sem=z_recv.at[0],
        device_id=(mate, t), device_id_type=MESH,
    ).wait_recv()
    weight_copies[0].wait()
    weight_copies[1].wait()
    for k in range(n_z):
        if k > 0:
            gathered(k)
        up_half(k)
        if k == 0:
            weight_copies[2].wait()
        if k + 2 < n_z:
            gather(k + 2)
        down_half(k)
        if k == 0:
            convolve()
        if k > 0:
            finish(k - 1)
        if k == 1 or n_z == 1:
            mixer_end()
    finish(n_z - 1)

    block = ret.at[rows_of(mate, cap), :]
    pltpu.make_async_remote_copy(
        src_ref=block, dst_ref=block, send_sem=y_send.at[0], recv_sem=y_recv.at[0],
        device_id=(mate, t), device_id_type=MESH,
    ).wait_recv()
    for k in range(1, n_z):
        for cc in range(2):
            block = ret.at[rows_of(((z + k) % n_z) * 2 + cc, cap), :]
            pltpu.make_async_remote_copy(
                src_ref=block, dst_ref=block, send_sem=y_send.at[2 * k + cc],
                recv_sem=y_recv.at[2 * k + cc], device_id=(mate, t), device_id_type=MESH,
            ).wait_recv()
    at = lax.broadcasted_iota(jnp.int32, (rows, slots), 1)
    l0 = logits_ref[:, 0:1]
    l1 = logits_ref[:, 1:2]
    first = jnp.dot(
        (at == place0).astype(f32).astype(bf16), ret[...], preferred_element_type=f32
    )
    second = jnp.dot(
        (at == place1).astype(f32).astype(bf16), ret[...], preferred_element_type=f32
    )
    out_ref[...] = (
        first * jax.nn.sigmoid(l0 - l1) + second * jax.nn.sigmoid(l1 - l0)
    ).astype(bf16)
    for copy in [mate_copy] + z_copies + ag_copies + rs_copies + y_copies + conv_copies:
        copy.wait_send()


def on_device(
    mixer_input, mixer_gain, glu_value_weight, glu_gate_weight, conv_taps, conv_bias,
    channel_gain, channel_shift, mixer_out_weight, expert_input, expert_gain, routes,
    route_logits, gate_weight, up_weight, down_weight,
):
    n_ep, n_tp = lax.axis_size("ep"), lax.axis_size("tp")
    rows, feat = expert_input.shape
    cap = 3 * rows // n_ep
    cap = -(-cap // 16) * 16
    units = gate_weight.shape[2]
    width = feat // n_tp
    n_z, peers, pair, slots = n_ep // 2, n_tp - 1, 2 * cap, n_ep * cap
    taken, chans, taps = mixer_input.shape[0], conv_taps.shape[0], conv_taps.shape[1]
    keep = -(-(taps - 1) // 16) * 16
    vmem = pl.BlockSpec(memory_space=pltpu.VMEM)
    hbm = pl.BlockSpec(memory_space=pl.ANY)
    dma = pltpu.SemaphoreType.DMA
    expert_output, mixer_output = pl.pallas_call(
        functools.partial(step_kernel, n_ep, n_tp, cap),
        out_shape=(
            jax.ShapeDtypeStruct((rows, width), bf16),
            jax.ShapeDtypeStruct((taken, mixer_out_weight.shape[1]), bf16),
        ),
        in_specs=[vmem] * 5 + [hbm] * 3 + [vmem] * 5 + [hbm] * 4,
        out_specs=(vmem, vmem),
        scratch_shapes=[
            pltpu.VMEM((feat, units), bf16),
            pltpu.VMEM((feat, units), bf16),
            pltpu.VMEM((units, feat), bf16),
            pltpu.VMEM((rows, feat), bf16),
            pltpu.VMEM((slots, width), bf16),
            pltpu.VMEM((cap, feat), bf16),
            pltpu.VMEM((slots, feat), bf16),
            pltpu.VMEM((pair, units), bf16),
            pltpu.VMEM((n_z * peers, pair, width), bf16),
            pltpu.VMEM((n_z, pair, width), bf16),
            pltpu.VMEM((n_z * peers, pair, width), bf16),
            pltpu.VMEM((n_z, pair, width), bf16),
            pltpu.VMEM((slots, width), bf16),
            dma((7,)),
            dma((n_ep,)),
            dma((n_ep,)),
            dma((n_z * peers,)),
            dma((n_z * peers,)),
            dma((n_z * peers,)),
            dma((n_z * peers,)),
            dma((n_ep,)),
            dma((n_ep,)),
            pltpu.VMEM(mixer_input.shape, bf16),
            pltpu.VMEM(glu_value_weight.shape, bf16),
            pltpu.VMEM(glu_gate_weight.shape, bf16),
            pltpu.VMEM(mixer_out_weight.shape, bf16),
            pltpu.VMEM((taken, chans), bf16),
            pltpu.VMEM((keep, chans), bf16),
            pltpu.VMEM((keep + taken, chans), f32),
            pltpu.VMEM((taken, chans), bf16),
            pltpu.VMEM((n_tp, taken, chans), bf16),
            dma((2,)),
            dma((peers,)),
            dma((peers,)),
        ],
        compiler_params=pltpu.CompilerParams(
            collective_id=0, has_side_effects=True, vmem_limit_bytes=48 * 1024 * 1024
        ),
        cost_estimate=pl.CostEstimate(
            flops=6 * slots * feat * units, bytes_accessed=6 * feat * units, transcendentals=0
        ),
    )(
        expert_input, expert_gain[None, :], routes, routes.T, route_logits,
        gate_weight, up_weight, down_weight,
        mixer_gain[None, :], conv_taps.T, conv_bias[None, :], channel_gain[None, :],
        channel_shift[None, :], mixer_input, glu_value_weight, glu_gate_weight, mixer_out_weight,
    )
    return (mixer_output, expert_output)


def solution(mesh):
    in_specs = (
        P("ep", None),
        P(),
        P("tp", None),
        P("tp", None),
        P("tp", None),
        P("tp"),
        P(),
        P(),
        P(None, "tp"),
        P("ep", None),
        P(),
        P("ep", None),
        P("ep", None),
        P("ep", None, "tp"),
        P("ep", None, "tp"),
        P("ep", "tp", None),
    )
    out_specs = (P("ep", "tp"), P("ep", "tp"))
    return jax.shard_map(
        on_device, mesh=mesh, in_specs=in_specs, out_specs=out_specs, check_vma=False
    )
```
